128 devices in a mesh: sp: 16 (over z, y), tp: 8 (over x, core).
Axes of the slice: x: 4, y: 4, z: 4, core: 2. Of those that a mesh axis runs over, the one named last changes fastest.
Arguments:
- skip_stream_vector: bfloat16 [16384, 2048], P(('sp', 'tp')), may hold values from -6 to 6
- probe_preactivation: bfloat16 [16384, 1024], P('sp', 'tp'), may hold values from -6 to 6
- retention_preactivation: bfloat16 [16384, 1024], P('sp', 'tp'), may hold values from -4.5 to 4.5
- content_vector: bfloat16 [16384, 1024], P('sp', 'tp'), may hold values from -6 to 6
- emission_preactivation: bfloat16 [16384, 1024], P('sp', 'tp'), may hold values from -6 to 6
- retention_slack: float32 [1024], P('tp'), may hold values from 0 to 0.12
- surge_rate: float32 [16384, 1024], P('sp', 'tp'), may hold values from -1.2 to 0
- subspace_scaling_factor: float32 [1024], P('tp'), may hold values from 0.1 to 1.9
- emission_matrix: bfloat16 [1024, 2048], replicated, may hold values from -0.1875 to 0.1875
- mlp_scaling_factor: float32 [2048], replicated, may hold values from 0.1 to 1.9
- switch_matrix: bfloat16 [2048, 5632], P('sp', 'tp'), may hold values from -0.125 to 0.125
- expansion_matrix: bfloat16 [2048, 5632], P('sp', 'tp'), may hold values from -0.125 to 0.125
- contraction_matrix: bfloat16 [5632, 2048], P('tp', 'sp'), may hold values from -0.078125 to 0.078125
Outputs:
- stream_out: bfloat16 [16384, 2048], P(('sp', 'tp'))
The draws below stay inside these ranges and needn't reach their ends.
All inputs are finite; a program needn't handle non-finite values.
Results may differ from the reference program's by a relative error of at most 0.017.
Values may be sent and summed in bfloat16 or wider, within the bound.
No kernel may reach another device: no remote copies, remote signals or barrier semaphores. Data moves between devices by JAX's collectives and lax.ppermute only.
A program may use at most 128 MiB of HBM per device.

```python
import jax
import jax.numpy as jnp
from jax import lax

D = 2048
HEADS = 8
HEAD_DIM = 128
FF = 5632
BLOCK = 64
TOK_DEV = 1024
D_HGRN = 1024
TOKENS = 16384
N_TP = 8


def draw_retention_slack(key, part):
    first_key, second_key, third_key = jax.random.split(jax.random.fold_in(key, 11), 3)
    ranking = jax.random.permutation(first_key, HEADS)
    slow_heads = ranking < HEADS // 2
    slow_gap = jnp.exp(jax.random.uniform(second_key, (HEADS, HEAD_DIM), jnp.float32, jnp.log(0.2), jnp.log(0.8))) / TOKENS
    fast_gap = jnp.exp(jax.random.uniform(third_key, (HEADS, HEAD_DIM), jnp.float32, jnp.log(0.04), jnp.log(0.12)))
    chosen = jnp.where(slow_heads[:, None], slow_gap, fast_gap)
    return jnp.minimum(chosen, 0.12).reshape(HEADS * HEAD_DIM)


def draw_retention_preactivation(key, part):
    first_key, second_key = jax.random.split(jax.random.fold_in(key, 21))
    noise = jnp.clip(0.8 * jax.random.normal(first_key, (TOKENS, HEADS * HEAD_DIM), jnp.float32), -3.0, 3.0)
    offsets = jax.random.uniform(second_key, (TOKENS // TOK_DEV, HEADS), jnp.float32, -1.2, 1.2)
    spread_rows = jnp.repeat(jnp.repeat(offsets, TOK_DEV, axis=0), HEAD_DIM, axis=1)
    return (noise + spread_rows).astype(jnp.bfloat16)


def draw_surge_rate(key, part):
    first_key, second_key = jax.random.split(jax.random.fold_in(key, 31))
    positions = jax.random.randint(first_key, (2, HEADS), 0, TOKENS)
    strength = jnp.log(jax.random.uniform(second_key, (2, HEADS), jnp.float32, 0.55, 0.8))
    places = jnp.arange(TOKENS, dtype=jnp.int32)[:, None, None]
    hits = jnp.sum(jnp.where(places == positions[None, :, :], strength[None, :, :], 0.0), axis=1)
    return jnp.repeat(hits, HEAD_DIM, axis=1)


def levels(rng, shape, pieces, low, largest):
    loudness, own = 1.0, jax.random.fold_in(rng, 6)
    for position, shards_of in pieces:
        draws = jnp.exp(jax.random.uniform(jax.random.fold_in(own, position), (shards_of,), jnp.float32, low / len(pieces), largest / len(pieces)))
        loudness = loudness * jnp.repeat(draws, shape[position] // shards_of).reshape([-1 if axis == position else 1 for axis in range(len(shape))])
    return loudness


def normal_values(own_key, extent, width, limit, shards=(), kind=jnp.bfloat16):
    drawn = width * jax.random.normal(own_key, extent, jnp.float32)
    if shards:
        drawn = drawn * levels(own_key, extent, shards, -0.22, 0.18)
    return jnp.clip(drawn, -limit, limit).astype(kind)


def setup_inputs(seed: int = 0) -> dict:
    key_of = jax.random.split(jax.random.key(seed), 14)
    return {
        "skip_stream_vector": normal_values(key_of[0], (TOKENS, D), 1.0, 6.0, ((0, 128),)),
        "probe_preactivation": normal_values(key_of[1], (TOKENS, D_HGRN), 1.0, 6.0, ((0, 16), (1, 8))),
        "retention_preactivation": draw_retention_preactivation(jax.random.fold_in(key_of[13], 71), 0),
        "content_vector": normal_values(key_of[3], (TOKENS, D_HGRN), 1.0, 6.0, ((0, 16), (1, 8))),
        "emission_preactivation": normal_values(key_of[4], (TOKENS, D_HGRN), 1.0, 6.0, ((0, 16), (1, 8))),
        "retention_slack": draw_retention_slack(jax.random.fold_in(key_of[13], 71), 0),
        "surge_rate": draw_surge_rate(jax.random.fold_in(key_of[13], 71), 0),
        "subspace_scaling_factor": jnp.clip(1.0 + 0.18 * jax.random.normal(key_of[7], (D_HGRN,), jnp.float32), 0.1, 1.9),
        "emission_matrix": normal_values(key_of[8], (D_HGRN, D), D_HGRN ** -0.5, 0.1875),
        "mlp_scaling_factor": jnp.clip(1.0 + 0.18 * jax.random.normal(key_of[9], (D,), jnp.float32), 0.1, 1.9),
        "switch_matrix": normal_values(key_of[10], (D, FF), D ** -0.5, 0.125, ((0, 16), (1, 8))),
        "expansion_matrix": normal_values(key_of[11], (D, FF), D ** -0.5, 0.125, ((0, 16), (1, 8))),
        "contraction_matrix": normal_values(key_of[12], (FF, D), FF ** -0.5, 0.078125, ((0, 8), (1, 16))),
    }


EPSILON = 1e-06
TOP_PRECISION = lax.Precision.HIGHEST

def block_step(carry, inputs):
    memory_state, offsets = carry
    query_block, input_gate_block, value_block, log_blk = inputs
    cumulative_decay = jnp.cumsum(log_blk, axis=1)
    length = log_blk.shape[1]
    carried_share = jnp.einsum('eia,eax->eix', query_block * jnp.exp(cumulative_decay), memory_state, precision=TOP_PRECISION)
    middle = cumulative_decay[:, length // 2, :][:, None, :]
    left_side = query_block * jnp.exp(cumulative_decay - middle)
    right_side = input_gate_block * jnp.exp(middle - cumulative_decay)
    causal = (jnp.arange(length)[:, None] >= jnp.arange(length)[None, :])[None, :, :]
    scores = jnp.einsum('htk,hsk->hts', left_side, right_side, precision=TOP_PRECISION)
    scores = jnp.where(causal, scores, 0.0)
    outputs = carried_share + jnp.einsum('hts,hsv->htv', scores, value_block, precision=TOP_PRECISION)
    closing_log_decay = cumulative_decay[:, -1, :]
    updated_memory_state = jnp.exp(closing_log_decay)[:, :, None] * memory_state + jnp.einsum('qnj,qnl->qjl', input_gate_block * jnp.exp(closing_log_decay[:, None, :] - cumulative_decay), value_block, precision=TOP_PRECISION)
    return ((updated_memory_state, offsets + closing_log_decay), (outputs, cumulative_decay + offsets[:, None, :]))

def split_blocks(values, heads_here):
    count = values.shape[0]
    return values.reshape(count // BLOCK, BLOCK, heads_here, HEAD_DIM).transpose(0, 2, 1, 3)

def admission_source_matrix(probe_preactivation, retention_preactivation, content_vector, retention_slack, surge_rate):
    query_act = jax.nn.silu(probe_preactivation.astype(jnp.float32))
    admission_factor = retention_slack[None, :] * jax.nn.sigmoid(-retention_preactivation.astype(jnp.float32))
    retention_logarithm = jnp.log1p(-admission_factor) + surge_rate
    return (query_act, admission_factor, content_vector.astype(jnp.float32), retention_logarithm)

def head_output(outputs, subspace_scaling_factor, emission_preactivation):
    count, heads_here = (outputs.shape[0], outputs.shape[1])
    squares = lax.optimization_barrier(jnp.mean(outputs * outputs, axis=-1, keepdims=True))
    scaled = outputs * lax.rsqrt(squares + EPSILON) * subspace_scaling_factor.reshape(heads_here, HEAD_DIM)
    scaled = scaled.reshape(count, heads_here * HEAD_DIM)
    return (scaled * jax.nn.silu(emission_preactivation.astype(jnp.float32))).astype(jnp.bfloat16)

def row_norm(stream, mlp_scaling_factor):
    streamf = stream.astype(jnp.float32)
    squares = lax.optimization_barrier(jnp.mean(streamf * streamf, axis=-1, keepdims=True))
    return (streamf * lax.rsqrt(squares + EPSILON) * mlp_scaling_factor).astype(jnp.bfloat16)

def reference(skip_stream_vector, probe_preactivation, retention_preactivation, content_vector, emission_preactivation, retention_slack, surge_rate, subspace_scaling_factor, emission_matrix, mlp_scaling_factor, switch_matrix, expansion_matrix, contraction_matrix):
    arranged_sources = admission_source_matrix(probe_preactivation, retention_preactivation, content_vector, retention_slack, surge_rate)
    block_list = tuple((split_blocks(item, HEADS) for item in arranged_sources))
    start_carry = (jnp.zeros((HEADS, HEAD_DIM, HEAD_DIM), jnp.float32), jnp.zeros((HEADS, HEAD_DIM), jnp.float32))
    _, (outputs, _) = lax.scan(block_step, start_carry, block_list)
    outputs = outputs.transpose(0, 2, 1, 3).reshape(TOKENS, HEADS, HEAD_DIM)
    mixed = head_output(outputs, subspace_scaling_factor, emission_preactivation)
    projected = jnp.dot(mixed, emission_matrix, preferred_element_type=jnp.float32)
    stream = (skip_stream_vector.astype(jnp.float32) + projected).astype(jnp.bfloat16)
    normed = row_norm(stream, mlp_scaling_factor)
    gate_proj = jnp.dot(normed, switch_matrix, preferred_element_type=jnp.float32)
    up_proj = jnp.dot(normed, expansion_matrix, preferred_element_type=jnp.float32)
    hidden = (jax.nn.silu(gate_proj) * up_proj).astype(jnp.bfloat16)
    slice_width = FF // N_TP
    summed = jnp.zeros((TOKENS, D), jnp.float32)
    for member in range(N_TP):
        lower = member * slice_width
        partial_sum = jnp.dot(hidden[:, lower:lower + slice_width], contraction_matrix[lower:lower + slice_width], preferred_element_type=jnp.float32)
        summed = summed + partial_sum.astype(jnp.bfloat16).astype(jnp.float32)
    return (stream.astype(jnp.float32) + summed).astype(jnp.bfloat16)
```

```python
import functools

import jax
import jax.numpy as jnp
from jax import lax
from jax.experimental import pallas as pl
from jax.experimental.pallas import tpu as pltpu
from jax.sharding import Mesh
from jax.sharding import PartitionSpec as P

HD = 128
BLOCK = 64
EPS = 1e-06
F32 = jnp.float32
BF16 = jnp.bfloat16
SP = ("z", "y")
TP = ("x", "c")
SIDE = 4


STEPS = (
    (((0, 0), (1, 0)), ((0, 0), (-1, 0)), ((0, 0), (0, 1)), ((0, 0), (0, -1))),
    (((0, 1), (1, 0)), ((0, -1), (-1, 0)), ((-1, 0), (0, 1)), ((1, 0), (0, -1))),
    (((1, 0), (1, 0)), ((-1, 1), (-1, 0)), ((0, 1), (0, 1)), ((1, -1), (0, -1))),
    (((1, -1), (1, 0)), ((2, 1), (0, 1)), ((-1, -1), (0, -1))),
)


def params(**kw):
    return pltpu.CompilerParams(vmem_limit_bytes=60 * 1024 * 1024, **kw)


def cost(flops, nbytes):
    return pl.CostEstimate(flops=int(flops), bytes_accessed=int(nbytes), transcendentals=0)


def sigmoid(x):
    return 1.0 / (1.0 + jnp.exp(-x))


def silu(x):
    return x / (1.0 + jnp.exp(-x))


def dot(a, b, dims):
    return lax.dot_general(a, b, (dims, ((), ())), preferred_element_type=F32)


NT = ((1,), (1,))
NN = ((1,), (0,))
TN = ((0,), (0,))


def wrap(v):
    return (v[0] % SIDE, v[1] % SIDE)


def plane_shift(x, d):
    pairs = []
    for z in range(SIDE):
        for y in range(SIDE):
            pairs.append((z * SIDE + y, (z + d[1]) % SIDE * SIDE + (y + d[0]) % SIDE))
    return lax.ppermute(x, SP, pairs)


def ring_shift(x, axis, k):
    return lax.ppermute(x, axis, [(i, (i + k) % SIDE) for i in range(SIDE)])


def line_shift(x, axis, k):
    return lax.ppermute(x, axis, [(i, i + k) for i in range(SIDE - k)])


def swap(x):
    return lax.ppermute(x, "c", [(0, 1), (1, 0)])


def state_kernel(ret_ref, val_ref, slack_ref, surge_ref, cum_ref, ig_ref, st_ref, msg_ref, off_ref):
    rows = ret_ref.shape[0]
    blocks = rows // BLOCK
    ig = slack_ref[...] * sigmoid(-ret_ref[...].astype(F32))
    lf = jnp.log1p(-ig) + surge_ref[...]
    ig_ref[...] = ig
    group = 4 * BLOCK
    r = lax.broadcasted_iota(jnp.int32, (group, group), 0)
    c = lax.broadcasted_iota(jnp.int32, (group, group), 1)
    tri = jnp.where((r >= c) & (r // BLOCK == c // BLOCK), 1.0, 0.0).astype(BF16)
    for g in range(rows // group):
        part = lf[g * group : (g + 1) * group]
        hi = part.astype(BF16)
        rest = part - hi.astype(F32)
        mid = rest.astype(BF16)
        low = (rest - mid.astype(F32)).astype(BF16)
        three = dot(tri, jnp.concatenate([hi, mid, low], axis=1), NN)
        cum_ref[g * group : (g + 1) * group, :] = (
            three[:, :HD] + three[:, HD : 2 * HD] + three[:, 2 * HD :]
        )
    state = jnp.zeros((HD, HD), F32)
    offset = jnp.zeros((1, HD), F32)
    for b in range(blocks):
        lo, hi = b * BLOCK, (b + 1) * BLOCK
        st_ref[b] = state.astype(BF16)
        off_ref[b : b + 1, :] = offset
        cum = cum_ref[lo:hi, :]
        last = cum[BLOCK - 1 : BLOCK, :]
        keys = (ig[lo:hi] * jnp.exp(last - cum)).astype(BF16)
        state = state * jnp.exp(last) + dot(val_ref[lo:hi, :], keys, TN)
        offset = offset + last
    msg_ref[0:HD, :] = state.astype(BF16)
    msg_ref[HD : HD + 16, :] = jnp.broadcast_to(jnp.exp(offset), (16, HD)).astype(BF16)


def local_kernel(q_ref, cum_ref, ig_ref, val_ref, st_ref, off_ref, out_ref, qd_ref):
    rows = q_ref.shape[0]
    group = 4 * BLOCK
    r = lax.broadcasted_iota(jnp.int32, (group, group), 0)
    c = lax.broadcasted_iota(jnp.int32, (group, group), 1)
    keep = (r >= c) & (r // BLOCK == c // BLOCK)
    for g in range(rows // group):
        lo, hi = g * group, (g + 1) * group
        q = silu(q_ref[lo:hi, :].astype(F32))
        cum = cum_ref[lo:hi, :].reshape(4, BLOCK, HD)
        rel = (cum - cum[:, BLOCK // 2 : BLOCK // 2 + 1, :]).reshape(group, HD)
        left = (q * jnp.exp(rel)).astype(BF16)
        right = (ig_ref[lo:hi, :] * jnp.exp(-rel)).astype(BF16)
        scores = jnp.where(keep, dot(left, right, NT), 0.0).astype(BF16)
        intra = dot(scores, val_ref[lo:hi, :], NN)
        decayed = q * jnp.exp(cum.reshape(group, HD))
        for k in range(4):
            b = g * 4 + k
            at = slice(k * BLOCK, (k + 1) * BLOCK)
            out_ref[b * BLOCK : (b + 1) * BLOCK, :] = intra[at] + dot(
                decayed[at].astype(BF16), st_ref[b], NT
            )
            qd_ref[b * BLOCK : (b + 1) * BLOCK, :] = (
                decayed[at] * jnp.exp(off_ref[b : b + 1, :])
            ).astype(BF16)


def read_msg(ref):
    return ref[0:HD, :].astype(F32), ref[HD : HD + 1, :].astype(F32)


def row_kernel(y_ref, own_ref, m1_ref, m2_ref, m3_ref, tot_ref, pre_ref):
    y = y_ref[0]
    own = read_msg(own_ref)
    back = [read_msg(m) for m in (m1_ref, m2_ref, m3_ref)]
    state, decay = jnp.zeros((HD, HD), F32), jnp.ones((1, HD), F32)
    for k in (3, 2, 1):
        s, d = back[k - 1]
        here = k <= y
        state = state * jnp.where(here, d, 1.0) + jnp.where(here, s, 0.0)
        decay = decay * jnp.where(here, d, 1.0)
    pre_ref[0:HD, :] = state
    pre_ref[HD : HD + 8, :] = jnp.broadcast_to(decay, (8, HD))
    state = state * own[1] + own[0]
    decay = decay * own[1]
    for k in (3, 2, 1):
        s, d = back[k - 1]
        here = k > y
        state = state * jnp.where(here, d, 1.0) + jnp.where(here, s, 0.0)
        decay = decay * jnp.where(here, d, 1.0)
    tot_ref[0:HD, :] = state.astype(BF16)
    tot_ref[HD : HD + 16, :] = jnp.broadcast_to(decay, (16, HD)).astype(BF16)


def mixed_kernel(z_ref, pre_ref, m1_ref, m2_ref, m3_ref, out_ref, qd_ref, gain_ref, em_ref, mixed_ref):
    z = z_ref[0]
    state = jnp.zeros((HD, HD), F32)
    for k, m in ((3, m3_ref), (2, m2_ref), (1, m1_ref)):
        s, d = read_msg(m)
        here = k <= z
        state = state * jnp.where(here, d, 1.0) + jnp.where(here, s, 0.0)
    state = state * pre_ref[HD : HD + 1, :] + pre_ref[0:HD, :]
    o = out_ref[...] + dot(qd_ref[...], state.astype(BF16), NT)
    squares = jnp.mean(o * o, axis=-1, keepdims=True)
    scaled = o * lax.rsqrt(squares + EPS) * gain_ref[...]
    mixed_ref[...] = (scaled * silu(em_ref[...].astype(F32))).astype(BF16)


def vmem(n):
    return [pl.BlockSpec(memory_space=pltpu.VMEM)] * n


SMEM = pl.BlockSpec(memory_space=pltpu.SMEM)


def recurrence(q_pre, ret, val, em, slack, surge, gain):
    rows = ret.shape[0]
    blocks = rows // BLOCK
    cum, ig, st, msg, off = pl.pallas_call(
        state_kernel,
        out_shape=(
            jax.ShapeDtypeStruct((rows, HD), F32),
            jax.ShapeDtypeStruct((rows, HD), F32),
            jax.ShapeDtypeStruct((blocks, HD, HD), BF16),
            jax.ShapeDtypeStruct((HD + 16, HD), BF16),
            jax.ShapeDtypeStruct((blocks, HD), F32),
        ),
        in_specs=vmem(4),
        out_specs=tuple(vmem(5)),
        compiler_params=params(),
        cost_estimate=cost(1e9, 2e6),
        name="state",
    )(ret, val, slack, surge)
    msgs = [ring_shift(msg, "y", k) for k in (1, 2, 3)]
    out, qd = pl.pallas_call(
        local_kernel,
        out_shape=(
            jax.ShapeDtypeStruct((rows, HD), F32),
            jax.ShapeDtypeStruct((rows, HD), BF16),
        ),
        in_specs=vmem(6),
        out_specs=tuple(vmem(2)),
        compiler_params=params(),
        cost_estimate=cost(1e9, 2e6),
        name="local",
    )(q_pre, cum, ig, val, st, off)
    tot, pre = pl.pallas_call(
        row_kernel,
        out_shape=(
            jax.ShapeDtypeStruct((HD + 16, HD), BF16),
            jax.ShapeDtypeStruct((HD + 8, HD), F32),
        ),
        in_specs=[SMEM] + vmem(4),
        out_specs=tuple(vmem(2)),
        compiler_params=params(),
        cost_estimate=cost(1e8, 2e5),
        name="rowtot",
    )(lax.axis_index("y").reshape(1).astype(jnp.int32), msg, *msgs)
    earlier = [line_shift(tot, "z", k) for k in (1, 2, 3)]
    return pl.pallas_call(
        mixed_kernel,
        out_shape=jax.ShapeDtypeStruct((rows, HD), BF16),
        in_specs=[SMEM] + vmem(8),
        out_specs=pl.BlockSpec(memory_space=pltpu.VMEM),
        compiler_params=params(),
        cost_estimate=cost(5e8, 2e6),
        name="mixed",
    )(lax.axis_index("z").reshape(1).astype(jnp.int32), pre, *earlier, out, qd, gain, em)


def project_kernel(ids_ref, *refs):
    mixed = refs[0:8]
    weights = refs[8:16]
    own = refs[16:20]
    near = refs[20:24]
    factor_ref, normed_ref, stream_ref = refs[24:27]
    g = pl.program_id(0)
    k = ids_ref[12]
    acc = None
    for h in range(4):
        lhs = jnp.concatenate([mixed[2 * h][...], mixed[2 * h + 1][...]], axis=1)
        rhs = jnp.concatenate([weights[2 * h][...], weights[2 * h + 1][...]], axis=0)
        term = dot(lhs, rhs, NN)
        acc = term if acc is None else acc + term

    def skip(side, which):
        out = side[0][...]
        for j in range(1, 4):
            out = jnp.where(which == j, side[j][...], out)
        return out

    mine = skip(own, g).astype(F32)
    theirs = skip(near, g).astype(F32)
    first = jnp.where(k == 0, mine, theirs)
    second = jnp.where(k == 0, theirs, mine)
    stream = (jnp.concatenate([first, second], axis=0) + acc).astype(BF16)
    wide = stream.astype(F32)
    squares = jnp.mean(wide * wide, axis=-1, keepdims=True)
    normed_ref[0] = (wide * lax.rsqrt(squares + EPS) * factor_ref[...]).astype(BF16)
    stream_ref[...] = stream


def project(ids, mixed, skips, near_skips, emission, factor):
    width = emission.shape[1]
    rows2 = 256

    def head_spec(h):
        return pl.BlockSpec((HD, width), lambda g, ids, h=h: (ids[4 + h], 0))

    grid = pltpu.PrefetchScalarGridSpec(
        num_scalar_prefetch=1,
        grid=(4,),
        in_specs=[pl.BlockSpec((rows2, HD), lambda g, ids: (ids[g], 0))] * 8
        + [head_spec(h) for h in range(8)]
        + [pl.BlockSpec((128, width), lambda g, ids: (0, 0))] * 8
        + [pl.BlockSpec((1, width), lambda g, ids: (0, 0))],
        out_specs=[
            pl.BlockSpec((1, rows2, width), lambda g, ids: (g, 0, 0)),
            pl.BlockSpec((rows2, width), lambda g, ids: (0, 0)),
        ],
    )
    return pl.pallas_call(
        project_kernel,
        grid_spec=grid,
        out_shape=(
            jax.ShapeDtypeStruct((4, rows2, width), BF16),
            jax.ShapeDtypeStruct((rows2, width), BF16),
        ),
        compiler_params=params(dimension_semantics=("arbitrary",)),
        cost_estimate=cost(4.3e9, 1.4e7),
        name="project",
    )(ids, *mixed, *([emission] * 8), *skips, *near_skips, factor)


def assemble_kernel(ids_ref, *refs):
    out_ref = refs[-1]
    for n, ref in enumerate(refs[:-1]):
        at = pl.multiple_of(ids_ref[n] * 128, 128)
        out_ref[:, pl.ds(at, 128)] = ref[...]


def assemble(ids, pieces):
    hidden = pieces[0].shape[0]
    return pl.pallas_call(
        assemble_kernel,
        out_shape=jax.ShapeDtypeStruct((hidden, 128 * len(pieces)), BF16),
        in_specs=[SMEM] + vmem(len(pieces)),
        out_specs=pl.BlockSpec(memory_space=pltpu.VMEM),
        compiler_params=params(),
        cost_estimate=cost(1e9, 6e6),
        name="assemble",
    )(ids, *pieces)


def ffn_kernel(ids_ref, x_ref, gu_ref, down_ref, mine_ref, theirs_ref, acc_ref, hid_ref, res_ref):
    step = pl.program_id(0)
    parts = x_ref.shape[0]
    rows = x_ref.shape[1]
    flat = parts * rows
    x = x_ref[...].reshape(flat, x_ref.shape[2])
    term = dot(x, gu_ref[...].reshape(-1, gu_ref.shape[2]), NN)

    @pl.when(step == 0)
    def _():
        acc_ref[...] = term

    @pl.when(step > 0)
    def _():
        acc_ref[...] += term

    @pl.when(step == pl.num_programs(0) - 1)
    def _():
        a = acc_ref[...]
        hid_ref[:, 0:640] = (silu(a[:, 0:640]) * a[:, 640:1280]).astype(BF16)
        tail = a[:, 1280:1408]
        hid_ref[:, 640:704] = (silu(tail[:, 0:64]) * tail[:, 64:128]).astype(BF16)
        k = ids_ref[12]
        res_ref[...] = dot(hid_ref[...], down_ref[...], NN).astype(BF16)
        for p in range(parts):
            own = pl.multiple_of(p * rows + k * 128, 128)
            other = pl.multiple_of(p * rows + (1 - k) * 128, 128)
            mine_ref[p] = res_ref[pl.ds(own, 128), :]
            theirs_ref[p] = res_ref[pl.ds(other, 128), :]


def ffn(ids, x, first, parts, gu, down):
    rows, width = x.shape[1], x.shape[2]
    chunk = 4
    steps = gu.shape[0] // chunk
    n = gu.shape[2]
    hidden = down.shape[0]
    assert first % parts == 0
    at = first // parts
    grid = pltpu.PrefetchScalarGridSpec(
        num_scalar_prefetch=1,
        grid=(steps,),
        in_specs=[
            pl.BlockSpec((parts, rows, width // steps), lambda s, ids: (at, 0, s)),
            pl.BlockSpec((chunk, 128, n), lambda s, ids: (s, 0, 0)),
            pl.BlockSpec((hidden, width), lambda s, ids: (0, 0)),
        ],
        out_specs=[pl.BlockSpec((parts, 128, width), lambda s, ids: (0, 0, 0))] * 2,
        scratch_shapes=[
            pltpu.VMEM((parts * rows, n), F32),
            pltpu.VMEM((parts * rows, hidden), BF16),
            pltpu.VMEM((parts * rows, width), BF16),
        ],
    )
    return pl.pallas_call(
        ffn_kernel,
        grid_spec=grid,
        out_shape=(jax.ShapeDtypeStruct((parts, 128, width), BF16),) * 2,
        compiler_params=params(dimension_semantics=("arbitrary",)),
        cost_estimate=cost(2.2e9 * parts, 1e7),
        name="ffn",
    )(ids, x, gu, down)


def on_device(skip, q_pre, ret, val, em, slack, surge, gain, emission, factor, gate, up, down):
    x, c = lax.axis_index("x"), lax.axis_index("c")
    y, z = lax.axis_index("y"), lax.axis_index("z")
    i32 = jnp.int32
    order = [(x + 2) % SIDE, (x + 1) % SIDE, (x + 3) % SIDE, x]
    heads = []
    for chip in order:
        heads += [2 * chip + c, 2 * chip + 1 - c]
    ids = jnp.stack([v.astype(i32) for v in order + heads + [c]])

    packed = jnp.concatenate([gate[:, :640], up[:, :640], gate[:, 640:], up[:, 640:]], axis=1)
    gu = lax.all_gather(packed, SP, axis=0)

    held = {(0, 0): down}
    for step in STEPS:
        for v, d in step:
            held[wrap((v[0] + d[0], v[1] + d[1]))] = plane_shift(held[wrap(v)], d)
    places = list(held)
    origin = jnp.stack(
        [((z - v[1]) % SIDE * SIDE + (y - v[0]) % SIDE).astype(i32) for v in places]
    )
    down_all = assemble(origin, [held[v] for v in places])

    skips = [ring_shift(skip, "x", 2), ring_shift(skip, "x", -1), ring_shift(skip, "x", 1), skip]
    near_skips = [swap(s) for s in skips]

    mixed = recurrence(
        q_pre, ret, val, em, slack.reshape(1, -1), surge, gain.reshape(1, -1)
    )
    far = [ring_shift(mixed, "x", 2), ring_shift(mixed, "x", -1), ring_shift(mixed, "x", 1), mixed]
    both = []
    for m in far:
        both += [m, swap(m)]
    normed, stream2 = project(ids, both, skips, near_skips, emission, factor.reshape(1, -1))
    stream = lax.dynamic_slice_in_dim(stream2, c * 128, 128, axis=0)

    half = skip.shape[1] // 2
    mine, theirs = ffn(ids, normed, 0, 1, gu, down_all)
    across = (mine[0].astype(F32) + swap(theirs)[0].astype(F32)).astype(BF16)
    from_left = ring_shift(across[:, :half], "x", 1)
    from_right = ring_shift(across[:, half:], "x", -1)

    mine1, theirs1 = ffn(ids, normed, 1, 1, gu, down_all)
    mine2, theirs2 = ffn(ids, normed, 2, 1, gu, down_all)
    got1, got2 = swap(theirs1)[0], swap(theirs2)[0]
    right = mine1[0].astype(F32) + got1.astype(F32)
    left = mine2[0].astype(F32) + got2.astype(F32)
    right = jnp.concatenate([right[:, :half] + from_left.astype(F32), right[:, half:]], axis=1)
    left = jnp.concatenate([left[:, :half], left[:, half:] + from_right.astype(F32)], axis=1)
    a = ring_shift(right.astype(BF16), "x", 1)
    b = ring_shift(left.astype(BF16), "x", -1)

    mine3, theirs3 = ffn(ids, normed, 3, 1, gu, down_all)
    summed = (
        mine3[0].astype(F32)
        + swap(theirs3)[0].astype(F32)
        + a.astype(F32)
        + b.astype(F32)
    )
    return (stream.astype(F32) + summed).astype(BF16)


def solution(mesh):
    split = Mesh(mesh.devices.reshape(SIDE, SIDE, SIDE, 2), SP + TP)
    return jax.shard_map(
        on_device,
        mesh=split,
        in_specs=(
            P(SP + TP, None),
            P(SP, TP),
            P(SP, TP),
            P(SP, TP),
            P(SP, TP),
            P(TP),
            P(SP, TP),
            P(TP),
            P(),
            P(),
            P(SP, TP),
            P(SP, TP),
            P(TP, SP),
        ),
        out_specs=P(SP + TP, None),
        check_vma=False,
    )
```

```python
import functools

import jax
import jax.numpy as jnp
from jax import lax
from jax.experimental import pallas as pl
from jax.experimental.pallas import tpu as pltpu
from jax.sharding import Mesh
from jax.sharding import PartitionSpec as P

HD = 128
BLOCK = 64
EPS = 1e-06
F32 = jnp.float32
BF16 = jnp.bfloat16
SP = ("z", "y")
TP = ("x", "c")
SIDE = 4


STEPS = (
    (((0, 0), (1, 0)), ((0, 0), (-1, 0)), ((0, 0), (0, 1)), ((0, 0), (0, -1))),
    (((0, 1), (1, 0)), ((0, -1), (-1, 0)), ((-1, 0), (0, 1)), ((1, 0), (0, -1))),
    (((1, 0), (1, 0)), ((-1, 1), (-1, 0)), ((0, 1), (0, 1)), ((1, -1), (0, -1))),
    (((1, -1), (1, 0)), ((2, 1), (0, 1)), ((-1, -1), (0, -1))),
)


def params(**kw):
    return pltpu.CompilerParams(vmem_limit_bytes=60 * 1024 * 1024, **kw)


def cost(flops, nbytes):
    return pl.CostEstimate(flops=int(flops), bytes_accessed=int(nbytes), transcendentals=0)


def sigmoid(x):
    return 1.0 / (1.0 + jnp.exp(-x))


def silu(x):
    return x / (1.0 + jnp.exp(-x))


def dot(a, b, dims):
    return lax.dot_general(a, b, (dims, ((), ())), preferred_element_type=F32)


NT = ((1,), (1,))
NN = ((1,), (0,))
TN = ((0,), (0,))


def wrap(v):
    return (v[0] % SIDE, v[1] % SIDE)


def plane_shift(x, d):
    pairs = []
    for z in range(SIDE):
        for y in range(SIDE):
            pairs.append((z * SIDE + y, (z + d[1]) % SIDE * SIDE + (y + d[0]) % SIDE))
    return lax.ppermute(x, SP, pairs)


def ring_shift(x, axis, k):
    return lax.ppermute(x, axis, [(i, (i + k) % SIDE) for i in range(SIDE)])


def line_shift(x, axis, k):
    return lax.ppermute(x, axis, [(i, i + k) for i in range(SIDE - k)])


def swap(x):
    return lax.ppermute(x, "c", [(0, 1), (1, 0)])


def state_kernel(ret_ref, val_ref, slack_ref, surge_ref, cum_ref, ig_ref, st_ref, msg_ref, off_ref):
    rows = ret_ref.shape[0]
    blocks = rows // BLOCK
    ig = slack_ref[...] * sigmoid(-ret_ref[...].astype(F32))
    lf = jnp.log1p(-ig) + surge_ref[...]
    ig_ref[...] = ig
    group = 4 * BLOCK
    r = lax.broadcasted_iota(jnp.int32, (group, group), 0)
    c = lax.broadcasted_iota(jnp.int32, (group, group), 1)
    tri = jnp.where((r >= c) & (r // BLOCK == c // BLOCK), 1.0, 0.0).astype(BF16)
    for g in range(rows // group):
        part = lf[g * group : (g + 1) * group]
        hi = part.astype(BF16)
        rest = part - hi.astype(F32)
        mid = rest.astype(BF16)
        low = (rest - mid.astype(F32)).astype(BF16)
        three = dot(tri, jnp.concatenate([hi, mid, low], axis=1), NN)
        cum_ref[g * group : (g + 1) * group, :] = (
            three[:, :HD] + three[:, HD : 2 * HD] + three[:, 2 * HD :]
        )
    state = jnp.zeros((HD, HD), F32)
    offset = jnp.zeros((1, HD), F32)
    for b in range(blocks):
        lo, hi = b * BLOCK, (b + 1) * BLOCK
        st_ref[b] = state.astype(BF16)
        off_ref[b : b + 1, :] = offset
        cum = cum_ref[lo:hi, :]
        last = cum[BLOCK - 1 : BLOCK, :]
        keys = (ig[lo:hi] * jnp.exp(last - cum)).astype(BF16)
        state = state * jnp.exp(last) + dot(val_ref[lo:hi, :], keys, TN)
        offset = offset + last
    msg_ref[0:HD, :] = state.astype(BF16)
    msg_ref[HD : HD + 16, :] = jnp.broadcast_to(jnp.exp(offset), (16, HD)).astype(BF16)


def local_kernel(q_ref, cum_ref, ig_ref, val_ref, st_ref, off_ref, out_ref, qd_ref):
    rows = q_ref.shape[0]
    group = 4 * BLOCK
    r = lax.broadcasted_iota(jnp.int32, (group, group), 0)
    c = lax.broadcasted_iota(jnp.int32, (group, group), 1)
    keep = (r >= c) & (r // BLOCK == c // BLOCK)
    for g in range(rows // group):
        lo, hi = g * group, (g + 1) * group
        q = silu(q_ref[lo:hi, :].astype(F32))
        cum = cum_ref[lo:hi, :].reshape(4, BLOCK, HD)
        rel = (cum - cum[:, BLOCK // 2 : BLOCK // 2 + 1, :]).reshape(group, HD)
        left = (q * jnp.exp(rel)).astype(BF16)
        right = (ig_ref[lo:hi, :] * jnp.exp(-rel)).astype(BF16)
        scores = jnp.where(keep, dot(left, right, NT), 0.0).astype(BF16)
        intra = dot(scores, val_ref[lo:hi, :], NN)
        decayed = q * jnp.exp(cum.reshape(group, HD))
        for k in range(4):
            b = g * 4 + k
            at = slice(k * BLOCK, (k + 1) * BLOCK)
            out_ref[b * BLOCK : (b + 1) * BLOCK, :] = intra[at] + dot(
                decayed[at].astype(BF16), st_ref[b], NT
            )
            qd_ref[b * BLOCK : (b + 1) * BLOCK, :] = (
                decayed[at] * jnp.exp(off_ref[b : b + 1, :])
            ).astype(BF16)


def read_msg(ref):
    return ref[0:HD, :].astype(F32), ref[HD : HD + 1, :].astype(F32)


def row_kernel(y_ref, own_ref, m1_ref, m2_ref, m3_ref, tot_ref, pre_ref):
    y = y_ref[0]
    own = read_msg(own_ref)
    back = [read_msg(m) for m in (m1_ref, m2_ref, m3_ref)]
    state, decay = jnp.zeros((HD, HD), F32), jnp.ones((1, HD), F32)
    for k in (3, 2, 1):
        s, d = back[k - 1]
        here = k <= y
        state = state * jnp.where(here, d, 1.0) + jnp.where(here, s, 0.0)
        decay = decay * jnp.where(here, d, 1.0)
    pre_ref[0:HD, :] = state
    pre_ref[HD : HD + 8, :] = jnp.broadcast_to(decay, (8, HD))
    state = state * own[1] + own[0]
    decay = decay * own[1]
    for k in (3, 2, 1):
        s, d = back[k - 1]
        here = k > y
        state = state * jnp.where(here, d, 1.0) + jnp.where(here, s, 0.0)
        decay = decay * jnp.where(here, d, 1.0)
    tot_ref[0:HD, :] = state.astype(BF16)
    tot_ref[HD : HD + 16, :] = jnp.broadcast_to(decay, (16, HD)).astype(BF16)


def mixed_kernel(
    ids_ref, pre_ref, m1_ref, m2_ref, m3_ref, out_ref, qd_ref, gain_ref, em_ref, mine_ref, theirs_ref, all_ref
):
    z, c = ids_ref[0], ids_ref[1]
    state = jnp.zeros((HD, HD), F32)
    for k, m in ((3, m3_ref), (2, m2_ref), (1, m1_ref)):
        s, d = read_msg(m)
        here = k <= z
        state = state * jnp.where(here, d, 1.0) + jnp.where(here, s, 0.0)
    state = state * pre_ref[HD : HD + 1, :] + pre_ref[0:HD, :]
    o = out_ref[...] + dot(qd_ref[...], state.astype(BF16), NT)
    squares = jnp.mean(o * o, axis=-1, keepdims=True)
    scaled = o * lax.rsqrt(squares + EPS) * gain_ref[...]
    all_ref[...] = (scaled * silu(em_ref[...].astype(F32))).astype(BF16)
    for chip in range(SIDE):
        own = pl.multiple_of(chip * 256 + c * 128, 128)
        other = pl.multiple_of(chip * 256 + (1 - c) * 128, 128)
        mine_ref[chip * 128 : (chip + 1) * 128, :] = all_ref[pl.ds(own, 128), :]
        theirs_ref[chip * 128 : (chip + 1) * 128, :] = all_ref[pl.ds(other, 128), :]


def vmem(n):
    return [pl.BlockSpec(memory_space=pltpu.VMEM)] * n


SMEM = pl.BlockSpec(memory_space=pltpu.SMEM)


def recurrence(q_pre, ret, val, em, slack, surge, gain):
    rows = ret.shape[0]
    blocks = rows // BLOCK
    cum, ig, st, msg, off = pl.pallas_call(
        state_kernel,
        out_shape=(
            jax.ShapeDtypeStruct((rows, HD), F32),
            jax.ShapeDtypeStruct((rows, HD), F32),
            jax.ShapeDtypeStruct((blocks, HD, HD), BF16),
            jax.ShapeDtypeStruct((HD + 16, HD), BF16),
            jax.ShapeDtypeStruct((blocks, HD), F32),
        ),
        in_specs=vmem(4),
        out_specs=tuple(vmem(5)),
        compiler_params=params(),
        cost_estimate=cost(1e9, 2e6),
        name="state",
    )(ret, val, slack, surge)
    msgs = [ring_shift(msg, "y", k) for k in (1, 2, 3)]
    out, qd = pl.pallas_call(
        local_kernel,
        out_shape=(
            jax.ShapeDtypeStruct((rows, HD), F32),
            jax.ShapeDtypeStruct((rows, HD), BF16),
        ),
        in_specs=vmem(6),
        out_specs=tuple(vmem(2)),
        compiler_params=params(),
        cost_estimate=cost(1e9, 2e6),
        name="local",
    )(q_pre, cum, ig, val, st, off)
    tot, pre = pl.pallas_call(
        row_kernel,
        out_shape=(
            jax.ShapeDtypeStruct((HD + 16, HD), BF16),
            jax.ShapeDtypeStruct((HD + 8, HD), F32),
        ),
        in_specs=[SMEM] + vmem(4),
        out_specs=tuple(vmem(2)),
        compiler_params=params(),
        cost_estimate=cost(1e8, 2e5),
        name="rowtot",
    )(lax.axis_index("y").reshape(1).astype(jnp.int32), msg, *msgs)
    earlier = [line_shift(tot, "z", k) for k in (1, 2, 3)]
    zc = jnp.stack([lax.axis_index("z"), lax.axis_index("c")]).astype(jnp.int32)
    return pl.pallas_call(
        mixed_kernel,
        out_shape=(jax.ShapeDtypeStruct((rows // 2, HD), BF16),) * 2,
        in_specs=[SMEM] + vmem(8),
        out_specs=tuple(vmem(2)),
        scratch_shapes=[pltpu.VMEM((rows, HD), BF16)],
        compiler_params=params(),
        cost_estimate=cost(5e8, 2e6),
        name="mixed",
    )(zc, pre, *earlier, out, qd, gain, em)


def pack_kernel(gate_ref, up_ref, down_ref, out_ref):
    for n in range(5):
        out_ref[0:128, n * 256 : n * 256 + 128] = gate_ref[:, n * 128 : (n + 1) * 128]
        out_ref[0:128, n * 256 + 128 : n * 256 + 256] = up_ref[:, n * 128 : (n + 1) * 128]
    out_ref[0:128, 1280:1408] = jnp.concatenate([gate_ref[:, 640:704], up_ref[:, 640:704]], axis=1)
    for n in range(11):
        out_ref[128:192, n * 128 : (n + 1) * 128] = down_ref[n * 64 : (n + 1) * 64, :]


def pack(gate, up, down):
    return pl.pallas_call(
        pack_kernel,
        out_shape=jax.ShapeDtypeStruct((192, 1408), BF16),
        in_specs=vmem(3),
        out_specs=pl.BlockSpec(memory_space=pltpu.VMEM),
        compiler_params=params(),
        cost_estimate=cost(1e8, 1.1e6),
        name="pack",
    )(gate, up, down)


def project_kernel(ids_ref, org_ref, *refs):
    mixed = refs[0:4]
    emission_ref = refs[4]
    skips = refs[5:9]
    factor_ref, normed_ref, stream_ref, skip_ref, norm_ref = refs[9:14]
    c = ids_ref[4]
    for n in range(4):
        at = pl.multiple_of(ids_ref[n] * 128, 128)
        skip_ref[pl.ds(at, 128), :] = skips[n][...]
    acc = skip_ref[...].astype(F32)
    for n in range(4):
        own = pl.multiple_of(ids_ref[n] * 256 + c * 128, 128)
        other = pl.multiple_of(ids_ref[n] * 256 + (1 - c) * 128, 128)
        rhs = jnp.concatenate(
            [emission_ref[pl.ds(own, 128), :], emission_ref[pl.ds(other, 128), :]], axis=0
        )
        acc = acc + dot(mixed[n][...], rhs, NN)
    stream = acc.astype(BF16)
    wide = stream.astype(F32)
    squares = jnp.mean(wide * wide, axis=-1, keepdims=True)
    norm_ref[...] = (wide * lax.rsqrt(squares + EPS) * factor_ref[...]).astype(BF16)
    skip_ref[...] = stream
    here = pl.multiple_of(ids_ref[3] * 128, 128)
    stream_ref[...] = skip_ref[pl.ds(here, 128), :]
    for n in range(16):
        at = pl.multiple_of(org_ref[n] * 128, 128)
        normed_ref[:, n * 128 : (n + 1) * 128] = norm_ref[:, pl.ds(at, 128)]


def project(ids, org, mixed, emission, skips, factor):
    width = emission.shape[1]
    rows = mixed[0].shape[0]
    return pl.pallas_call(
        project_kernel,
        out_shape=(
            jax.ShapeDtypeStruct((rows, width), BF16),
            jax.ShapeDtypeStruct((128, width), BF16),
        ),
        in_specs=[SMEM, SMEM] + vmem(10),
        out_specs=tuple(vmem(2)),
        scratch_shapes=[pltpu.VMEM((rows, width), BF16), pltpu.VMEM((rows, width), BF16)],
        compiler_params=params(),
        cost_estimate=cost(2.2e9, 1.4e7),
        name="project",
    )(ids, org, *mixed, emission, *skips, factor)


def down_part(ids_ref, org_ref, blocks, base, hid_ref, chip, out_refs, part):
    at = pl.multiple_of(ids_ref[chip] * 128, 128)
    also = pl.multiple_of(ids_ref[chip] * 128 + 512, 128)
    lhs = jnp.concatenate([hid_ref[pl.ds(at, 128), :], hid_ref[pl.ds(also, 128), :]], axis=0)
    for n in range(0, 16, 2):
        sides = []
        for ref in blocks[n : n + 2]:
            sides.append(
                jnp.concatenate(
                    [ref[base : base + 64, k * 128 : (k + 1) * 128] for k in range(11)], axis=0
                )
            )
        res = dot(lhs, jnp.concatenate(sides, axis=1), NN).astype(BF16)
        for k in range(2):
            to = pl.multiple_of(org_ref[n + k] * 128, 128)
            for row, ref in enumerate(out_refs):
                ref[part, :, pl.ds(to, 128)] = res[
                    row * 128 : (row + 1) * 128, k * 128 : (k + 1) * 128
                ]


def up_kernel(ids_ref, org_ref, x1_ref, x2_ref, *refs):
    blocks = refs[0:16]
    hid_ref, mine_ref, theirs_ref = refs[16:19]
    half = x1_ref.shape[0]

    def tile(at, size):
        for row, x_ref in enumerate((x1_ref, x2_ref)):
            acc = None
            for n in range(0, 16, 2):
                rhs = jnp.concatenate(
                    [blocks[n][0:128, pl.ds(at, size)], blocks[n + 1][0:128, pl.ds(at, size)]],
                    axis=0,
                )
                term = dot(x_ref[:, n * 128 : (n + 2) * 128], rhs, NN)
                acc = term if acc is None else acc + term
            w = size // 2
            yield row * half, (silu(acc[:, :w]) * acc[:, w:]).astype(BF16)

    def body(n, carry):
        at = pl.multiple_of(n * 256, 256)
        to = pl.multiple_of(n * 128, 128)
        for row, val in tile(at, 256):
            hid_ref[row : row + half, pl.ds(to, 128)] = val
        return carry

    lax.fori_loop(0, 5, body, 0)
    for row, val in tile(1280, 128):
        hid_ref[row : row + half, 640:704] = val
    down_part(ids_ref, org_ref, blocks, 128, hid_ref, 0, (mine_ref, theirs_ref), 0)


def feed_up(ids, org, x1, x2, blocks):
    rows = x1.shape[0] * 2
    width = x1.shape[1]
    return pl.pallas_call(
        up_kernel,
        out_shape=(jax.ShapeDtypeStruct((rows, 704), BF16),)
        + (jax.ShapeDtypeStruct((1, 128, width), BF16),) * 2,
        in_specs=[SMEM, SMEM] + vmem(18),
        out_specs=tuple(vmem(3)),
        compiler_params=params(),
        cost_estimate=cost(6.6e9, 1.4e7),
        name="feed_up",
    )(ids, org, x1, x2, *blocks)


def down_kernel(chips, ids_ref, org_ref, hid_ref, *refs):
    blocks = refs[0:16]
    for part, chip in enumerate(chips):
        down_part(ids_ref, org_ref, blocks, 0, hid_ref, chip, refs[16:18], part)


def feed_down(ids, org, hid, blocks, chips):
    width = 16 * 128
    whole = pl.BlockSpec(hid.shape, lambda i: (0, 0))
    piece = pl.BlockSpec((64, 1408), lambda i: (2, 0))
    out = (len(chips), 128, width)
    return pl.pallas_call(
        functools.partial(down_kernel, chips),
        grid=(1,),
        out_shape=(jax.ShapeDtypeStruct(out, BF16),) * 2,
        in_specs=[SMEM, SMEM, whole] + [piece] * 16,
        out_specs=[pl.BlockSpec(out, lambda i: (0, 0, 0))] * 2,
        compiler_params=params(),
        cost_estimate=cost(0.8e9 * len(chips), 5e6),
        name="feed_down",
    )(ids, org, hid, *blocks)


def on_device(skip, q_pre, ret, val, em, slack, surge, gain, emission, factor, gate, up, down):
    x, c = lax.axis_index("x"), lax.axis_index("c")
    y, z = lax.axis_index("y"), lax.axis_index("z")
    i32 = jnp.int32
    order = [(x + 2) % SIDE, (x + 1) % SIDE, (x + 3) % SIDE, x]
    ids = jnp.stack([v.astype(i32) for v in order + [c]])

    held = {(0, 0): pack(gate, up, down)}
    for step in STEPS:
        for v, d in step:
            held[wrap((v[0] + d[0], v[1] + d[1]))] = plane_shift(held[wrap(v)], d)
    places = list(held)
    blocks = [held[v] for v in places]
    org = jnp.stack(
        [((z - v[1]) % SIDE * SIDE + (y - v[0]) % SIDE).astype(i32) for v in places]
    )

    skips = [ring_shift(skip, "x", 2), ring_shift(skip, "x", -1), ring_shift(skip, "x", 1), skip]

    mine, theirs = recurrence(
        q_pre, ret, val, em, slack.reshape(1, -1), surge, gain.reshape(1, -1)
    )
    mixed = jnp.concatenate([mine, swap(theirs)], axis=1)
    mixed = [ring_shift(mixed, "x", 2), ring_shift(mixed, "x", -1), ring_shift(mixed, "x", 1), mixed]
    normed, stream = project(ids, org, mixed, emission, skips, factor.reshape(1, -1))

    half = skip.shape[1] // 2
    hid, mine, theirs = feed_up(ids, org, normed, swap(normed), blocks)
    across = (mine[0].astype(F32) + swap(theirs)[0].astype(F32)).astype(BF16)
    from_left = ring_shift(across[:, :half], "x", 1)
    from_right = ring_shift(across[:, half:], "x", -1)

    mine, theirs = feed_down(ids, org, hid, blocks, (1, 2))
    sums = mine.astype(F32) + swap(theirs).astype(F32)
    right = jnp.concatenate(
        [sums[0, :, :half] + from_left.astype(F32), sums[0, :, half:]], axis=1
    )
    left = jnp.concatenate(
        [sums[1, :, :half], sums[1, :, half:] + from_right.astype(F32)], axis=1
    )
    a = ring_shift(right.astype(BF16), "x", 1)
    b = ring_shift(left.astype(BF16), "x", -1)

    mine, theirs = feed_down(ids, org, hid, blocks, (3,))
    summed = (
        mine[0].astype(F32) + swap(theirs)[0].astype(F32) + a.astype(F32) + b.astype(F32)
    )
    return (stream.astype(F32) + summed).astype(BF16)


def solution(mesh):
    split = Mesh(mesh.devices.reshape(SIDE, SIDE, SIDE, 2), SP + TP)
    return jax.shard_map(
        on_device,
        mesh=split,
        in_specs=(
            P(SP + TP, None),
            P(SP, TP),
            P(SP, TP),
            P(SP, TP),
            P(SP, TP),
            P(TP),
            P(SP, TP),
            P(TP),
            P(),
            P(),
            P(SP, TP),
            P(SP, TP),
            P(TP, SP),
        ),
        out_specs=P(SP + TP, None),
        check_vma=False,
    )
```
